32 devices in a mesh: ep: 4 (over y, x), tp: 8 (over z, core).
Axes of the slice: x: 2, y: 2, z: 4, core: 2. Of those that a mesh axis runs over, the one named last changes fastest.
Arguments:
- tokens: bfloat16 [128, 2048], P(('ep', 'tp')), may hold values from -6 to 6
- lengths: int32 [128], P(('ep', 'tp')), may hold values from 64 to 1024
- cache_latent: bfloat16 [128, 1024, 512], P(('ep', 'tp')), may hold values from -6 to 6
- cache_rope_key: bfloat16 [128, 1024, 32], P(('ep', 'tp')), may hold values from -1000 to 1000
- route_ids: int32 [128, 4], P('ep'), may hold values from 0 to 31, all different within a row; in each aligned block of 32 rows (0 to 31, 32 to 63, ...) at most 8 rows name the same one
- route_weights: float32 [128, 4], P('ep'), may hold values from 0.2 to 2
- attn_gain: float32 [2048], replicated, may hold values from 0.1 to 1.9
- w_query_nope: bfloat16 [2048, 16, 64], P(None, 'tp'), may hold values from -0.125 to 0.125
- w_query_rope: bfloat16 [2048, 16, 32], P(None, 'tp'), may hold values from -0.125 to 0.125
- w_latent_down: bfloat16 [2048, 512], P(None, 'tp'), may hold values from -0.125 to 0.125
- w_key_rope: bfloat16 [2048, 32], replicated, may hold values from -0.125 to 0.125
- latent_gain: float32 [512], replicated, may hold values from 0.1 to 1.9
- w_key_up: bfloat16 [512, 16, 64], P(None, 'tp'), may hold values from -0.75 to 0.75
- w_value_up: bfloat16 [512, 16, 64], P(None, 'tp'), may hold values from -0.25 to 0.25
- w_attn_out: bfloat16 [16, 64, 2048], P('tp'), may hold values from -0.1875 to 0.1875
- ffn_gain: float32 [2048], replicated, may hold values from 0.1 to 1.9
- expert_gate: bfloat16 [32, 2048, 512], P(('ep', 'tp')), may hold values from -0.125 to 0.125
- expert_up: bfloat16 [32, 2048, 512], P(('ep', 'tp')), may hold values from -0.125 to 0.125
- expert_down: bfloat16 [32, 512, 2048], P(('ep', 'tp')), may hold values from -0.25 to 0.25
- shared_gate: bfloat16 [2048, 512], P(None, 'tp'), may hold values from -0.125 to 0.125
- shared_up: bfloat16 [2048, 512], P(None, 'tp'), may hold values from -0.125 to 0.125
- shared_down: bfloat16 [512, 2048], P('tp'), may hold values from -0.25 to 0.25
- dense_gate: bfloat16 [2048, 1024], P(None, 'tp'), may hold values from -0.125 to 0.125
- dense_up: bfloat16 [2048, 1024], P(None, 'tp'), may hold values from -0.125 to 0.125
- dense_down: bfloat16 [1024, 2048], P('tp'), may hold values from -0.1875 to 0.1875
- branch_gate: bfloat16 [2048], replicated, may hold values from -0.125 to 0.125
Outputs:
- mixed: bfloat16 [128, 2048], P(('ep', 'tp'))
- new_latent: bfloat16 [128, 512], P(('ep', 'tp'))
- new_rope_key: bfloat16 [128, 32], P(('ep', 'tp'))
The draws below stay inside these ranges and needn't reach their ends.
Inputs may be any that keep to these rules, and one draw needn't show every extreme that they name: `route_ids`: in each aligned block of 32 rows, no expert is named by more than 8 of the block's rows, a bound that some block reaches. Each row names 4 different experts.
All inputs are finite; a program needn't handle non-finite values.
Results may differ from the reference program's by a relative error of at most 0.025.
Values may be sent and summed in bfloat16 or wider, within the bound.
A program may use at most 64 MiB of HBM per device.

```python
import math
import jax
import jax.numpy as jnp
import numpy as np
from jax import lax

D = 2048
HEADS = 16
NOPE = 64
ROPE = 32
VHEAD = 64
LATENT = 512
EXPERT_FF = 512
SHARED_FF = 512
DENSE_FF = 1024
TOP_K = 4
LEN = 1024
GROUP = 32
SEQS = 128
EXPERTS = 32
CAP = 8
N_EP = 4


def draw_cache_rope_key(key, part):
    values = jnp.clip(jax.random.normal(key, (SEQS, LEN, ROPE), jnp.float32), -6.0, 6.0)
    return values.astype(jnp.bfloat16)


def plant(array, rng, low, top_value):
    longest = array.shape.index(max(array.shape))
    spots = []
    for shift in (0, 1):
        where = [jax.random.randint(jax.random.fold_in(rng, axis), (), 0, length) for axis, length in enumerate(array.shape)]
        where[longest] = (where[longest] + shift) % array.shape[longest]
        spots.append(tuple(where))
    return array.at[spots[0]].set(low).at[spots[1]].set(top_value)


def steps_of(own_key, dims, cuts, low, high):
    gain, own = 1.0, jax.random.fold_in(own_key, 6)
    for axis_at, blocks in cuts:
        heights = jnp.exp(jax.random.uniform(jax.random.fold_in(own, axis_at), (blocks,), jnp.float32, low / len(cuts), high / len(cuts)))
        gain = gain * jnp.repeat(heights, dims[axis_at] // blocks).reshape([-1 if axis == axis_at else 1 for axis in range(len(dims))])
    return gain


def assign_block(rng, own, number, rows, number_of, top, most, skew):
    ranking = jax.random.permutation(rng, number_of)
    packed, common = load_shares(number_of, rows * top, most, skew, True), load_shares(number_of, rows * top, most, skew, False)
    places = jnp.arange(number_of)

    def named(sizes, rotation):
        used = int((sizes > 0).sum())
        fixed = max(1, used // 4)
        moved = fixed + (places - fixed + rotation * (used - fixed)) % max(1, number_of - fixed)
        return jnp.zeros((number_of,), jnp.int32).at[ranking[jnp.where(places < fixed, places, moved)]].set(jnp.asarray(sizes, jnp.int32))

    sizes = jnp.where(number % 4 == 0, named(packed, number // 4), named(common, number - number // 4 - 1))
    mixed = jax.random.permutation(jax.random.fold_in(own, 3), number_of)
    source_of, taker = mixed[0:number_of // 2 * 2:2], mixed[1:number_of // 2 * 2:2]
    slack = jnp.minimum(sizes[source_of] - 1, most - sizes[taker]) // 2
    slack = jnp.where((source_of == ranking[0]) | (taker == ranking[0]) | (sizes[taker] == 0), 0, jnp.maximum(slack, 0))
    moved = jax.random.randint(jax.random.fold_in(own, 4), (number_of // 2,), 0, 1 << 20) % (slack + 1)
    sizes = sizes.at[source_of].add(-moved).at[taker].add(moved)
    members = jnp.searchsorted(jnp.cumsum(sizes), jnp.arange(rows * top), side="right").astype(jnp.int32)
    grid = members.reshape(top, rows).T
    grid = grid[jax.random.permutation(jax.random.fold_in(own, 1), rows)]
    rotation = jax.random.randint(jax.random.fold_in(own, 2), (rows, 1), 0, top)
    return jnp.take_along_axis(grid, (jnp.arange(top)[None, :] + rotation) % top, axis=1)


def load_shares(count, total, most, slope, full):
    portions = [(1 << 20) // math.isqrt(rank ** slope) + 1 for rank in range(1, count + 1)]
    largest = most if full else min(most, max(-(-total // count), total * portions[0] // sum(portions)))
    least = 1 if total - largest >= count - 1 else 0
    given, rest = [largest] + [least] * (count - 1), total - largest - least * (count - 1)
    while rest > 0:
        candidates = [i for i in range(1, count) if given[i] < largest] or [i for i in range(1, count) if given[i] < most]
        pool, remaining = sum([portions[i] for i in candidates]), rest
        for i in candidates:
            addition = min(most - given[i], max(1, remaining * portions[i] // pool), rest)
            given[i] = given[i] + addition
            rest = rest - addition
    return np.array(given)


def bell_draw(own_key, shape, deviation, reach, pieces=(), held_as=jnp.bfloat16):
    level = steps_of(own_key, shape, pieces, -0.22, 0.18) if pieces else 1.0
    entries = jax.random.normal(own_key, shape, jnp.float32) * deviation * level
    return jnp.minimum(jnp.maximum(entries, -reach), reach).astype(held_as)


def setup_inputs(seed: int = 0) -> dict:
    key_list = jax.random.split(jax.random.key(seed), 27)
    tokens = bell_draw(key_list[0], (SEQS, D), 1.0, 6.0, ((0, 32),))
    lengths = plant(jax.random.randint(key_list[1], (SEQS,), LEN // 16, LEN + 1), jax.random.fold_in(key_list[1], 1), LEN // 16, LEN).astype(jnp.int32)
    cache_latent = bell_draw(key_list[2], (SEQS, LEN, LATENT), 1.0, 6.0, ((0, 32),))
    cache_rope_key = draw_cache_rope_key(jax.random.fold_in(key_list[26], 71), 0)
    route_ids_keys = jax.random.split(jax.random.fold_in(key_list[4], 1), SEQS // GROUP)
    route_ids_turns = jax.random.permutation(jax.random.fold_in(key_list[4], 3), SEQS // GROUP)
    route_ids = jax.vmap(lambda own, number: assign_block(jax.random.fold_in(key_list[4], 2), own, number, GROUP, EXPERTS, TOP_K, CAP, 2))(route_ids_keys, route_ids_turns).reshape((SEQS, TOP_K))
    route_weights = jnp.clip(jnp.exp(math.log(2.0) - 2.3025851 * jax.random.uniform(key_list[5], (SEQS, TOP_K), jnp.float32) ** steps_of(key_list[5], (SEQS, TOP_K), ((0, 4),), -0.2, 0.2)), 0.2, 2.0)
    attn_gain = jnp.clip(1.0 + 0.18 * jax.random.normal(key_list[6], (D,), jnp.float32), 0.1, 1.9)
    w_query_nope = bell_draw(key_list[7], (D, HEADS, NOPE), D ** -0.5, 0.125, ((1, 8),))
    w_query_rope = bell_draw(key_list[8], (D, HEADS, ROPE), D ** -0.5, 0.125, ((1, 8),))
    w_latent_down = bell_draw(key_list[9], (D, LATENT), D ** -0.5, 0.125, ((1, 8),))
    w_key_rope = bell_draw(key_list[10], (D, ROPE), D ** -0.5, 0.125)
    latent_gain = jnp.clip(1.0 + 0.18 * jax.random.normal(key_list[11], (LATENT,), jnp.float32), 0.1, 1.9)
    w_key_up = bell_draw(key_list[12], (LATENT, HEADS, NOPE), NOPE ** -0.5, 0.75, ((1, 8),))
    w_value_up = bell_draw(key_list[13], (LATENT, HEADS, VHEAD), LATENT ** -0.5, 0.25, ((1, 8),))
    w_attn_out = bell_draw(key_list[14], (HEADS, VHEAD, D), (HEADS * VHEAD) ** -0.5, 0.1875, ((0, 8),))
    ffn_gain = jnp.clip(1.0 + 0.18 * jax.random.normal(key_list[15], (D,), jnp.float32), 0.1, 1.9)
    expert_gate = bell_draw(key_list[16], (EXPERTS, D, EXPERT_FF), D ** -0.5, 0.125, ((0, 32),))
    expert_up = bell_draw(key_list[17], (EXPERTS, D, EXPERT_FF), D ** -0.5, 0.125, ((0, 32),))
    expert_down = bell_draw(key_list[18], (EXPERTS, EXPERT_FF, D), EXPERT_FF ** -0.5, 0.25, ((0, 32),))
    shared_gate = bell_draw(key_list[19], (D, SHARED_FF), D ** -0.5, 0.125, ((1, 8),))
    shared_up = bell_draw(key_list[20], (D, SHARED_FF), D ** -0.5, 0.125, ((1, 8),))
    shared_down = bell_draw(key_list[21], (SHARED_FF, D), SHARED_FF ** -0.5, 0.25, ((0, 8),))
    dense_gate = bell_draw(key_list[22], (D, DENSE_FF), D ** -0.5, 0.125, ((1, 8),))
    dense_up = bell_draw(key_list[23], (D, DENSE_FF), D ** -0.5, 0.125, ((1, 8),))
    dense_down = bell_draw(key_list[24], (DENSE_FF, D), DENSE_FF ** -0.5, 0.1875, ((0, 8),))
    branch_gate = bell_draw(key_list[25], (D,), D ** -0.5, 0.125)
    return dict(tokens=tokens, lengths=lengths, cache_latent=cache_latent, cache_rope_key=cache_rope_key, route_ids=route_ids, route_weights=route_weights, attn_gain=attn_gain, w_query_nope=w_query_nope, w_query_rope=w_query_rope, w_latent_down=w_latent_down, w_key_rope=w_key_rope, latent_gain=latent_gain, w_key_up=w_key_up, w_value_up=w_value_up, w_attn_out=w_attn_out, ffn_gain=ffn_gain, expert_gate=expert_gate, expert_up=expert_up, expert_down=expert_down, shared_gate=shared_gate, shared_up=shared_up, shared_down=shared_down, dense_gate=dense_gate, dense_up=dense_up, dense_down=dense_down, branch_gate=branch_gate)


epsilon = 1e-06
rope_base = 10000.0

def norm_rows(values, scales):
    values = values.astype(jnp.float32)
    factor = lax.rsqrt(lax.optimization_barrier(jnp.mean(values * values, axis=-1, keepdims=True)) + epsilon)
    return values * factor * scales.astype(jnp.float32)

def rotate(values, positions):
    half_dim = values.shape[-1] // 2
    frequencies = rope_base ** (-jnp.arange(half_dim).astype(jnp.float32) / half_dim)
    angles = positions.astype(jnp.float32)[:, None] * frequencies[None, :]
    bcast_shape = (angles.shape[0],) + (1,) * (values.ndim - 2) + (half_dim,)
    cosine = jnp.cos(angles).reshape(bcast_shape)
    sine_val = jnp.sin(angles).reshape(bcast_shape)
    first_half = values[..., :half_dim].astype(jnp.float32)
    second_half = values[..., half_dim:].astype(jnp.float32)
    return jnp.concatenate([first_half * cosine - second_half * sine_val, first_half * sine_val + second_half * cosine], axis=-1)

def swiglu(inputs, gate_w, up_w):
    gate_val = jnp.dot(inputs, gate_w, preferred_element_type=jnp.float32)
    up_val = jnp.dot(inputs, up_w, preferred_element_type=jnp.float32)
    return (jax.nn.silu(gate_val) * up_val).astype(jnp.bfloat16)

def attend(group_data):
    q_lat, q_rot, lat_new, rope_new, lat_cache, rope_cache, seq_len = group_data
    head_scale = (NOPE + ROPE) ** (-0.5)
    scores = jnp.einsum('bhr,blr->bhl', q_lat.astype(jnp.float32), lat_cache.astype(jnp.float32))
    scores = scores + jnp.einsum('bhe,ble->bhl', q_rot.astype(jnp.float32), rope_cache.astype(jnp.float32))
    scores = scores * head_scale
    in_range = jnp.arange(lat_cache.shape[1], dtype=jnp.int32)[None, None, :] < seq_len[:, None, None]
    scores = jnp.where(in_range, scores, -jnp.inf)
    own_score = jnp.einsum('bhr,br->bh', q_lat.astype(jnp.float32), lat_new.astype(jnp.float32))
    own_score = (own_score + jnp.einsum('bhe,be->bh', q_rot.astype(jnp.float32), rope_new.astype(jnp.float32))) * head_scale
    peak_score = jnp.maximum(lax.optimization_barrier(jnp.max(scores, axis=-1)), own_score)
    past_exp = jnp.exp(scores - peak_score[..., None])
    own_exp = jnp.exp(own_score - peak_score)
    total_exp = lax.optimization_barrier(jnp.sum(past_exp, axis=-1)) + own_exp
    past_weight = (past_exp / total_exp[..., None]).astype(jnp.bfloat16)
    own_weight = (own_exp / total_exp).astype(jnp.bfloat16)
    out_latent = jnp.einsum('bhl,blr->bhr', past_weight.astype(jnp.float32), lat_cache.astype(jnp.float32))
    out_latent = out_latent + own_weight.astype(jnp.float32)[..., None] * lat_new.astype(jnp.float32)[:, None, :]
    return out_latent.astype(jnp.bfloat16)

def reference(tokens, lengths, cache_latent, cache_rope_key, route_ids, route_weights, attn_gain, w_query_nope, w_query_rope, w_latent_down, w_key_rope, latent_gain, w_key_up, w_value_up, w_attn_out, ffn_gain, expert_gate, expert_up, expert_down, shared_gate, shared_up, shared_down, dense_gate, dense_up, dense_down, branch_gate):
    seq_count, model_width = tokens.shape
    head_count = w_query_nope.shape[1]
    normed = norm_rows(tokens, attn_gain).astype(jnp.bfloat16)
    query_nope = jnp.dot(normed, w_query_nope.reshape(model_width, -1), preferred_element_type=jnp.float32)
    query_nope = query_nope.astype(jnp.bfloat16).reshape(seq_count, head_count, -1)
    query_latent = jnp.einsum('shn,rhn->shr', query_nope.astype(jnp.float32), w_key_up.astype(jnp.float32)).astype(jnp.bfloat16)
    query_rope = jnp.dot(normed, w_query_rope.reshape(model_width, -1), preferred_element_type=jnp.float32)
    query_rope = query_rope.astype(jnp.bfloat16).reshape(seq_count, head_count, -1)
    latent_raw = jnp.dot(normed, w_latent_down, preferred_element_type=jnp.float32).astype(jnp.bfloat16)
    new_latent = norm_rows(latent_raw, latent_gain).astype(jnp.bfloat16)
    new_rope = rotate(jnp.dot(normed, w_key_rope, preferred_element_type=jnp.float32), lengths).astype(jnp.bfloat16)
    query_rot = rotate(query_rope, lengths).astype(jnp.bfloat16)
    grouped = tuple((member.reshape((N_EP, GROUP) + member.shape[1:]) for member in (query_latent, query_rot, new_latent, new_rope, cache_latent, cache_rope_key, lengths)))
    out_latent = lax.map(attend, grouped).reshape(seq_count, head_count, -1)
    head_values = jnp.einsum('shr,rhv->shv', out_latent.astype(jnp.float32), w_value_up.astype(jnp.float32)).astype(jnp.bfloat16)
    after_attn = tokens.astype(jnp.float32) + jnp.dot(head_values.reshape(seq_count, -1), w_attn_out.reshape(-1, model_width), preferred_element_type=jnp.float32)
    ffn_in = norm_rows(after_attn, ffn_gain).astype(jnp.bfloat16)
    shared_term = jnp.dot(swiglu(ffn_in, shared_gate, shared_up), shared_down, preferred_element_type=jnp.float32)
    branch_mix = jax.nn.sigmoid(jnp.dot(ffn_in, branch_gate, preferred_element_type=jnp.float32))
    dense_term = branch_mix[:, None] * jnp.dot(swiglu(ffn_in, dense_gate, dense_up), dense_down, preferred_element_type=jnp.float32)
    top_count = route_ids.shape[1]
    flat_expert = route_ids.reshape(-1).astype(jnp.int32)
    flat_row = jnp.arange(seq_count * top_count, dtype=jnp.int32) // top_count
    expert_hits = (flat_expert[:, None] == jnp.arange(EXPERTS, dtype=jnp.int32)[None, :]).astype(jnp.int32)
    expert_hits = expert_hits.reshape(N_EP, GROUP * top_count, EXPERTS)
    earlier = jnp.cumsum(expert_hits, axis=1) - expert_hits
    rank_in = lax.optimization_barrier(jnp.sum(earlier * expert_hits, axis=2)).reshape(-1).astype(jnp.int32)
    slot_index = (flat_row // GROUP * CAP + rank_in).astype(jnp.int32)
    slot_table = jnp.full((EXPERTS, N_EP * CAP), seq_count, jnp.int32).at[flat_expert, slot_index].set(flat_row)
    padded_in = jnp.concatenate([ffn_in, jnp.zeros((1, model_width), jnp.bfloat16)], axis=0)

    def one_expert(expert_data):
        row_ids, gate_w, up_w, down_w = expert_data
        act_val = swiglu(padded_in[row_ids], gate_w, up_w)
        return jnp.dot(act_val, down_w, preferred_element_type=jnp.float32).astype(jnp.bfloat16)
    expert_out = lax.map(one_expert, (slot_table, expert_gate, expert_up, expert_down))
    picked = expert_out[flat_expert, slot_index].astype(jnp.float32).reshape(seq_count, top_count, model_width)
    routed = lax.optimization_barrier(jnp.sum(picked * route_weights.astype(jnp.float32)[:, :, None], axis=1))
    mixed = (after_attn + routed + shared_term + dense_term).astype(jnp.bfloat16)
    return (mixed, new_latent, new_rope)
```

```python
import functools

import jax
import jax.numpy as jnp
from jax import lax
from jax.experimental import pallas as pl
from jax.experimental.pallas import tpu as pltpu
from jax.sharding import PartitionSpec as P

epsilon = 1e-06
rope_base = 10000.0
lanes = 128
F32 = jnp.float32
BF16 = jnp.bfloat16
MESH = pl.DeviceIdType.MESH


def nn(a, b):
    return lax.dot_general(a, b, (((1,), (0,)), ((), ())), preferred_element_type=F32)


def nt(a, b):
    return lax.dot_general(a, b, (((1,), (1,)), ((), ())), preferred_element_type=F32)


def tn(a, b):
    return lax.dot_general(a, b, (((0,), (0,)), ((), ())), preferred_element_type=F32)


def join(pieces):
    return pieces[0] if len(pieces) == 1 else jnp.concatenate(pieces, axis=0)


def rows_of(ref, count):
    return join([ref[i].astype(F32) for i in range(count)])


def factor_of(values):
    return lax.rsqrt(jnp.mean(values * values, axis=-1, keepdims=True) + epsilon)


def silu(v):
    return v / (1.0 + jnp.exp(-v))


def lane_block(values, column, width):
    base, offset = column // lanes * lanes, column % lanes
    block = values[:, base : base + lanes]
    if offset:
        block = pltpu.roll(block, lanes - offset, 1)
    lane = lax.broadcasted_iota(jnp.int32, block.shape, 1)
    return jnp.where(lane < width, block, 0.0)


def turn(values, cosine, sine, half):
    lane = lax.broadcasted_iota(jnp.int32, values.shape, 1)
    swapped = jnp.where(
        lane < half, -pltpu.roll(values, lanes - half, 1), pltpu.roll(values, half, 1)
    )
    return values * cosine + swapped * sine


def layer(
    sizes,
    consts, tab, tokens, ids, wts,
    wqn, wqr, wld, wkr, cl, cr, wku, wvu, wo, sg, su, dg, du, sd, dd, eg, eu, ed,
    mixed, newlat, newrope,
    v_in, v_kr, v_cl, v_cr, v_ku, v_vu, v_wo, v_sg, v_su, v_dg, v_du, v_sd, v_dd, v_eg, v_eu, v_ed,
    agx, sendq, recvq, sendo, recvo, senda, recva, agf, sende, recve, sendr, recvr, sendf, recvf,
    kr_pad, w_sem, tp_send, tp_recv, ep_send, ep_recv,
):
    T, EP, own, H, nope, rope, latent, cap, scale = sizes
    group = T * own
    R = H * own
    me_t = lax.axis_index("tp")
    me_e = lax.axis_index("ep")
    lat_w = wld.shape[0]

    barrier = pltpu.get_barrier_semaphore()
    for k in range(1, T):
        pl.semaphore_signal(
            barrier, inc=1, device_id=(me_e, lax.rem(me_t + k, T)), device_id_type=MESH
        )
    for k in range(1, EP):
        pl.semaphore_signal(
            barrier, inc=1, device_id=(lax.rem(me_e + k, EP), me_t), device_id_type=MESH
        )

    n_q, n_r = H * nope, H * rope
    pairs = [
        (wqn, v_in.at[pl.ds(0, n_q)]),
        (wqr, v_in.at[pl.ds(n_q, n_r)]),
        (wld, v_in.at[pl.ds(n_q + n_r, lat_w)]),
        (wkr, v_kr),
        (wku, v_ku),
    ]
    first_cl = len(pairs)
    pairs += [(cl.at[b], v_cl.at[b]) for b in range(own)]
    first_rest = len(pairs)
    pairs += [(cr, v_cr), (wvu, v_vu), (wo, v_wo)]
    first_ffn = len(pairs)
    pairs += [
        (sg, v_sg), (su, v_su), (dg, v_dg), (du, v_du), (sd, v_sd), (dd, v_dd),
        (eg, v_eg), (eu, v_eu), (ed, v_ed),
    ]
    loads = [
        pltpu.make_async_copy(src, dst, w_sem.at[i]) for i, (src, dst) in enumerate(pairs)
    ]
    for load in loads:
        load.start()

    sends = []

    def tp_exchange(phase, source, target):
        out = []
        for k in range(1, T):
            peer = lax.rem(me_t + k, T)
            out.append(
                pltpu.make_async_remote_copy(
                    src_ref=source(peer),
                    dst_ref=target.at[me_t],
                    send_sem=tp_send.at[phase, k],
                    recv_sem=tp_recv.at[phase, k],
                    device_id=(me_e, peer),
                    device_id_type=MESH,
                )
            )
        for c in out:
            c.start()
        sends.extend(out)
        return out

    def ep_exchange(phase, source, target):
        out = []
        for k in range(1, EP):
            peer = lax.rem(me_e + k, EP)
            out.append(
                pltpu.make_async_remote_copy(
                    src_ref=source.at[peer],
                    dst_ref=target.at[me_e],
                    send_sem=ep_send.at[phase, k],
                    recv_sem=ep_recv.at[phase, k],
                    device_id=(peer, me_t),
                    device_id_type=MESH,
                )
            )
        for c in out:
            c.start()
        sends.extend(out)
        return out

    def arrive(copies):
        for c in copies:
            c.wait_recv()

    x = tokens[...].astype(F32)
    normed = (x * factor_of(x) * consts[0:1, :]).astype(BF16)
    agx[me_t] = normed
    pl.semaphore_wait(barrier, T - 1 + EP - 1)
    step = tp_exchange(0, lambda peer: agx.at[me_t], agx)

    slots = EP * cap
    slot = lax.broadcasted_iota(jnp.int32, (slots, group), 0)
    block = jnp.zeros((slots, group), jnp.int32)
    for j in range(1, EP):
        block = block + jnp.where(slot >= j * cap, 1, 0)
    expert = block * T + me_t
    place = (slot - block * cap).astype(F32)
    hit = jnp.zeros((slots, group), F32)
    weight = jnp.zeros((slots, group), F32)
    for k in range(ids.shape[0]):
        same = ids[k : k + 1, :] == expert
        hit = hit + jnp.where(same, 1.0, 0.0)
        weight = weight + jnp.where(same, wts[k : k + 1, :], 0.0)
    upper = jnp.where(
        lax.broadcasted_iota(jnp.int32, (group, group), 0)
        < lax.broadcasted_iota(jnp.int32, (group, group), 1),
        1.0,
        0.0,
    ).astype(BF16)
    rank = nn(hit.astype(BF16), upper)
    dispatch = jnp.where(rank == place, hit, 0.0)
    weight = weight * dispatch
    weight_hi = weight.astype(BF16)
    weight_lo = (weight - weight_hi.astype(F32)).astype(BF16)
    dispatch = dispatch.astype(BF16)

    for i in range(first_cl):
        loads[i].wait()
    cosine, sine = tab[0], tab[1]
    kr_pad[...] = jnp.zeros_like(kr_pad)
    kr_pad[:, 0:rope] = nt(normed, v_kr[...])
    new_rope = turn(kr_pad[...], cosine[0:own], sine[0:own], rope // 2).astype(BF16)
    newrope[...] = new_rope[:, 0:rope]

    arrive(step)
    rows = rows_of(agx, T).astype(BF16)
    proj = nt(rows, v_in[...])
    q_lat = [
        nn(lane_block(proj, h * nope, nope)[:, 0:nope].astype(BF16), v_ku[h]) for h in range(H)
    ]
    q_rope = [lane_block(proj, n_q + h * rope, rope) for h in range(H)]
    lat_part = lane_block(proj, n_q + n_r, lat_w)
    for u in range(T):
        cut = slice(own * u, own * (u + 1))
        sendq[u, :, 0:latent] = join([q[cut] for q in q_lat]).astype(BF16)
        sendq[u, :, latent : latent + lanes] = join([q[cut] for q in q_rope]).astype(BF16)
        sendq[u, :, latent + lanes : latent + 2 * lanes] = join([lat_part[cut]] * H).astype(BF16)
    step = tp_exchange(1, lambda peer: sendq.at[peer], recvq)
    recvq[me_t] = sendq[me_t]
    for i in range(first_cl, first_ffn):
        loads[i].wait()
    arrive(step)

    queries = rows_of(recvq, T)
    q_all = queries[:, 0:latent].astype(BF16)
    q_rot = turn(queries[:, latent : latent + lanes], cosine, sine, rope // 2).astype(BF16)
    per = lanes // lat_w
    blocks = []
    for j in range(T // per):
        total = None
        for i in range(per):
            piece = queries[R * (j * per + i) : R * (j * per + i) + own, latent + lanes :]
            if i:
                piece = pltpu.roll(piece, i * lat_w, 1)
            total = piece if total is None else total + piece
        blocks.append(total)
    raw = blocks[0] if len(blocks) == 1 else jnp.concatenate(blocks, axis=1)
    new_latent = (raw * factor_of(raw) * consts[3:4, 0:latent]).astype(BF16)
    newlat[...] = new_latent
    lat_rows = join([new_latent.astype(F32)] * (T * H))
    rope_rows = join([new_rope.astype(F32)] * (T * H))
    own_score = (
        jnp.sum(q_all.astype(F32) * lat_rows, axis=-1, keepdims=True)
        + jnp.sum(q_rot.astype(F32) * rope_rows, axis=-1, keepdims=True)
    ) * scale
    length = tab[2][:, 0:1]
    which = tab[3][:, 0:1]
    scores = None
    for b in range(own):
        part = nt(q_all, v_cl[b]) + nn(q_rot[:, 0:rope], v_cr[b])
        scores = part if scores is None else jnp.where(which == float(b), part, scores)
    position = lax.broadcasted_iota(jnp.int32, scores.shape, 1).astype(F32)
    scores = jnp.where(position < length, scores * scale, -jnp.inf)
    peak = jnp.maximum(jnp.max(scores, axis=-1, keepdims=True), own_score)
    past = jnp.exp(scores - peak)
    own_exp = jnp.exp(own_score - peak)
    total = jnp.sum(past, axis=-1, keepdims=True) + own_exp
    past = (past / total).astype(BF16)
    own_weight = (own_exp / total).astype(BF16).astype(F32)
    mixed_lat = None
    for b in range(own):
        part = nn(past, v_cl[b])
        mixed_lat = part if mixed_lat is None else jnp.where(which == float(b), part, mixed_lat)
    mixed_lat = mixed_lat + own_weight * lat_rows
    for u in range(T):
        sendo[u] = mixed_lat[R * u : R * (u + 1)].astype(BF16)
    step = tp_exchange(2, lambda peer: sendo.at[peer], recvo)
    recvo[me_t] = sendo[me_t]
    arrive(step)

    back = rows_of(recvo, T).astype(BF16)
    part = None
    for h in range(H):
        values = nt(back, v_vu[h])
        values = join(
            [values[R * u + own * h : R * u + own * (h + 1)] for u in range(T)]
        ).astype(BF16)
        term = nn(values, v_wo[h])
        part = term if part is None else part + term
    for u in range(T):
        senda[u] = part[own * u : own * (u + 1)].astype(BF16)
    step = tp_exchange(3, lambda peer: senda.at[peer], recva)
    recva[me_t] = senda[me_t]
    arrive(step)
    after = tokens[...].astype(F32)
    for u in range(T):
        after = after + recva[u].astype(F32)
    agf[me_t] = (after * factor_of(after) * consts[1:2, :]).astype(BF16)
    step = tp_exchange(4, lambda peer: agf.at[me_t], agf)
    for i in range(first_ffn, len(loads)):
        loads[i].wait()
    arrive(step)

    rows32 = rows_of(agf, T)
    rows = rows32.astype(BF16)
    outgoing = nn(dispatch, rows)
    for j in range(EP):
        sende[j] = outgoing[cap * j : cap * (j + 1)].astype(BF16)
    step = ep_exchange(0, sende, recve)
    recve[me_e] = sende[me_e]

    act = (silu(nt(rows, v_sg[...])) * nt(rows, v_su[...])).astype(BF16)
    ffn = nn(act, v_sd[...])
    gate = jnp.sum(rows32 * consts[2:3, :], axis=-1, keepdims=True)
    gate = 1.0 / (1.0 + jnp.exp(-gate))
    act = (silu(nn(rows, v_dg[...])) * nn(rows, v_du[...])).astype(BF16)
    ffn = ffn + gate * nn(act, v_dd[...])

    arrive(step)
    routed = rows_of(recve, EP).astype(BF16)
    act = (silu(nn(routed, v_eg[...])) * nn(routed, v_eu[...])).astype(BF16)
    result = nn(act, v_ed[...])
    for j in range(EP):
        sendr[j] = result[cap * j : cap * (j + 1)].astype(BF16)
    step = ep_exchange(1, sendr, recvr)
    recvr[me_e] = sendr[me_e]
    arrive(step)
    returned = rows_of(recvr, EP).astype(BF16)
    ffn = ffn + (tn(weight_hi, returned) + tn(weight_lo, returned))
    for u in range(T):
        sendf[u] = ffn[own * u : own * (u + 1)].astype(BF16)
    step = tp_exchange(5, lambda peer: sendf.at[peer], recvf)
    recvf[me_t] = sendf[me_t]
    arrive(step)
    for u in range(T):
        after = after + recvf[u].astype(F32)
    mixed[...] = after.astype(BF16)
    for c in sends:
        c.wait_send()


def local(
    tokens, lengths, cache_latent, cache_rope_key, route_ids, route_weights, attn_gain,
    w_query_nope, w_query_rope, w_latent_down, w_key_rope, latent_gain, w_key_up, w_value_up,
    w_attn_out, ffn_gain, expert_gate, expert_up, expert_down, shared_gate, shared_up,
    shared_down, dense_gate, dense_up, dense_down, branch_gate,
):
    own, width = tokens.shape
    T = lax.axis_size("tp")
    EP = lax.axis_size("ep")
    H, nope = w_query_nope.shape[1:]
    rope = w_query_rope.shape[2]
    latent = cache_latent.shape[2]
    top = route_ids.shape[1]
    assert expert_gate.shape[0] == 1
    cap = max(2, (2 * own * top + EP - 1) // EP)
    R = H * own
    half = rope // 2

    frequencies = rope_base ** (-jnp.arange(half).astype(F32) / half)
    angles = lengths.astype(F32)[:, None] * frequencies[None, :]
    pad = ((0, 0), (0, lanes - rope))
    cosine = jnp.pad(jnp.tile(jnp.cos(angles), (1, 2)), pad)
    sine = jnp.pad(jnp.tile(jnp.sin(angles), (1, 2)), pad)
    length = jnp.broadcast_to(lengths.astype(F32)[:, None], (own, lanes))
    which = jnp.broadcast_to(jnp.arange(own, dtype=F32)[:, None], (own, lanes))
    tab = jnp.stack([cosine, sine, length, which])
    tab = jnp.tile(tab, (1, T * H, 1))
    consts = jnp.stack(
        [
            attn_gain,
            ffn_gain,
            branch_gate.astype(F32),
            jnp.pad(latent_gain, (0, width - latent)),
        ]
    )

    operands = (
        consts,
        tab,
        tokens,
        route_ids.T,
        route_weights.T,
        w_query_nope.transpose(1, 2, 0).reshape(H * nope, width),
        w_query_rope.transpose(1, 2, 0).reshape(H * rope, width),
        w_latent_down.T,
        w_key_rope.T,
        cache_latent,
        cache_rope_key.transpose(0, 2, 1),
        w_key_up.transpose(1, 2, 0),
        w_value_up.transpose(1, 2, 0),
        w_attn_out,
        shared_gate.T,
        shared_up.T,
        dense_gate,
        dense_up,
        shared_down,
        dense_down,
        expert_gate[0],
        expert_up[0],
        expert_down[0],
    )
    big = operands[5:]
    v_in = pltpu.VMEM((sum(o.shape[0] for o in big[:3]), width), BF16)
    weights = [v_in] + [pltpu.VMEM(o.shape, BF16) for o in big[3:]]
    q_width = latent + 2 * lanes

    def comm(*shape):
        return pltpu.VMEM(shape, BF16)

    buffers = [
        comm(T, own, width),
        comm(T, R, q_width), comm(T, R, q_width),
        comm(T, R, latent), comm(T, R, latent),
        comm(T, own, width), comm(T, own, width),
        comm(T, own, width),
        comm(EP, cap, width), comm(EP, cap, width),
        comm(EP, cap, width), comm(EP, cap, width),
        comm(T, own, width), comm(T, own, width),
        pltpu.VMEM((own, lanes), F32),
    ]
    n_loads = len(big) + own - 1
    sems = [
        pltpu.SemaphoreType.DMA((n_loads,)),
        pltpu.SemaphoreType.DMA((6, T)),
        pltpu.SemaphoreType.DMA((6, T)),
        pltpu.SemaphoreType.DMA((2, EP)),
        pltpu.SemaphoreType.DMA((2, EP)),
    ]
    sizes = (T, EP, own, H, nope, rope, latent, cap, (nope + rope) ** (-0.5))
    vmem = pl.BlockSpec(memory_space=pltpu.VMEM)
    return pl.pallas_call(
        functools.partial(layer, sizes),
        out_shape=(
            jax.ShapeDtypeStruct((own, width), BF16),
            jax.ShapeDtypeStruct((own, latent), BF16),
            jax.ShapeDtypeStruct((own, rope), BF16),
        ),
        in_specs=[vmem] * 5 + [pl.BlockSpec(memory_space=pl.ANY)] * len(big),
        out_specs=(vmem, vmem, vmem),
        scratch_shapes=weights + buffers + sems,
        compiler_params=pltpu.CompilerParams(collective_id=0, has_side_effects=True),
    )(*operands)


def solution(mesh):
    both = ("ep", "tp")
    in_specs = (
        P(both, None),
        P(both),
        P(both, None, None),
        P(both, None, None),
        P("ep", None),
        P("ep", None),
        P(),
        P(None, "tp", None),
        P(None, "tp", None),
        P(None, "tp"),
        P(),
        P(),
        P(None, "tp", None),
        P(None, "tp", None),
        P("tp", None, None),
        P(),
        P(both, None, None),
        P(both, None, None),
        P(both, None, None),
        P(None, "tp"),
        P(None, "tp"),
        P("tp", None),
        P(None, "tp"),
        P(None, "tp"),
        P("tp", None),
        P(),
    )
    out_specs = (P(both, None), P(both, None), P(both, None))
    return jax.shard_map(local, mesh=mesh, in_specs=in_specs, out_specs=out_specs, check_vma=False)
```

```python
import functools

import jax
import jax.numpy as jnp
import numpy as np
from jax import lax
from jax.experimental import pallas as pl
from jax.experimental.pallas import tpu as pltpu
from jax.sharding import PartitionSpec as P

epsilon = 1e-06
rope_base = 10000.0
lanes = 128
F32 = jnp.float32
BF16 = jnp.bfloat16
MESH = pl.DeviceIdType.MESH


def nn(a, b):
    return lax.dot_general(a, b, (((1,), (0,)), ((), ())), preferred_element_type=F32)


def nt(a, b):
    return lax.dot_general(a, b, (((1,), (1,)), ((), ())), preferred_element_type=F32)


def tn(a, b):
    return lax.dot_general(a, b, (((0,), (0,)), ((), ())), preferred_element_type=F32)


def join(pieces):
    return pieces[0] if len(pieces) == 1 else jnp.concatenate(pieces, axis=0)


def flipped(index, mask, count):
    out = index
    bit = 1
    while bit < count:
        if mask & bit:
            out = out + bit - 2 * bit * (index // bit % 2)
        bit *= 2
    return out


def flat(ref):
    return jnp.concatenate([ref[i : i + 1, :] for i in range(ref.shape[0])], axis=1)


def spread(values, count):
    rows = values.shape[0]
    return join(
        [jnp.broadcast_to(values[b : b + 1], (count, values.shape[1])) for b in range(rows)]
    )


def rows_of(ref, count):
    return join([ref[i].astype(F32) for i in range(count)])


def factor_of(values):
    return lax.rsqrt(jnp.mean(values * values, axis=-1, keepdims=True) + epsilon)


def silu(v):
    return v / (1.0 + jnp.exp(-v))


def lane_block(values, column, width):
    base, offset = column // lanes * lanes, column % lanes
    block = values[:, base : base + lanes]
    if offset:
        block = pltpu.roll(block, lanes - offset, 1)
    lane = lax.broadcasted_iota(jnp.int32, block.shape, 1)
    return jnp.where(lane < width, block, 0.0)


def turn(values, cosine, sine, half):
    lane = lax.broadcasted_iota(jnp.int32, values.shape, 1)
    swapped = jnp.where(
        lane < half, -pltpu.roll(values, lanes - half, 1), pltpu.roll(values, half, 1)
    )
    return values * cosine + swapped * sine


def layer(
    sizes,
    turns, tokens, ids, wts, attn_gain, ffn_gain, latent_gain, branch_gate, lengths,
    wqn, wqr, wld, wkr, cl, cr, wku, wvu, wo, sg, su, dg, du, sd, dd, eg, eu, ed,
    mixed, newlat, newrope,
    v_in, v_kr, v_cl, v_cr, v_ku, v_vu, v_wo, v_sg, v_su, v_dg, v_du, v_sd, v_dd, v_eg, v_eu, v_ed,
    agx, sendq, recvq, sendo, recvo, senda, recva, agf, sende, recve, sendr, recvr, sendf, recvf,
    kr_pad, w_sem, tp_send, tp_recv, ep_send, ep_recv,
):
    T, EP, own, H, nope, rope, latent, cap, scale = sizes
    group = T * own
    R = H * own
    me_t = lax.axis_index("tp")
    me_e = lax.axis_index("ep")
    lat_w = wld.shape[0]

    barrier = pltpu.get_barrier_semaphore()
    for k in range(1, T):
        pl.semaphore_signal(
            barrier, inc=1, device_id=(me_e, flipped(me_t, k, T)), device_id_type=MESH
        )
    for k in range(1, EP):
        pl.semaphore_signal(
            barrier, inc=1, device_id=(flipped(me_e, k, EP), me_t), device_id_type=MESH
        )

    n_q, n_r = H * nope, H * rope
    pairs = [
        (wqn, v_in.at[pl.ds(0, n_q)]),
        (wqr, v_in.at[pl.ds(n_q, n_r)]),
        (wld, v_in.at[pl.ds(n_q + n_r, lat_w)]),
        (wkr, v_kr),
        (wku, v_ku),
    ]
    first_cl = len(pairs)
    pairs += [(cl.at[b], v_cl.at[b]) for b in range(own)]
    first_rest = len(pairs)
    pairs += [(cr, v_cr), (wvu, v_vu), (wo, v_wo)]
    first_ffn = len(pairs)
    pairs += [
        (sg, v_sg), (su, v_su), (dg, v_dg), (du, v_du), (sd, v_sd), (dd, v_dd),
        (eg, v_eg), (eu, v_eu), (ed, v_ed),
    ]
    loads = [
        pltpu.make_async_copy(src, dst, w_sem.at[i]) for i, (src, dst) in enumerate(pairs)
    ]
    for load in loads:
        load.start()

    sends = []

    def tp_exchange(phase, source, target):
        out = []
        for k in range(T - 1, 0, -1):
            peer = flipped(me_t, k, T)
            out.append(
                pltpu.make_async_remote_copy(
                    src_ref=source(peer),
                    dst_ref=target.at[me_t],
                    send_sem=tp_send.at[phase, k],
                    recv_sem=tp_recv.at[phase, k],
                    device_id=(me_e, peer),
                    device_id_type=MESH,
                )
            )
        for c in out:
            c.start()
        sends.extend(out)
        return out

    def ep_exchange(phase, source, target):
        out = []
        for k in range(EP - 1, 0, -1):
            peer = flipped(me_e, k, EP)
            out.append(
                pltpu.make_async_remote_copy(
                    src_ref=source.at[peer],
                    dst_ref=target.at[me_e],
                    send_sem=ep_send.at[phase, k],
                    recv_sem=ep_recv.at[phase, k],
                    device_id=(peer, me_t),
                    device_id_type=MESH,
                )
            )
        for c in out:
            c.start()
        sends.extend(out)
        return out

    def arrive(copies):
        for c in copies:
            c.wait_recv()

    x = tokens[...].astype(F32)
    normed = (x * factor_of(x) * flat(attn_gain[...])).astype(BF16)
    agx[me_t] = normed
    pl.semaphore_wait(barrier, T - 1 + EP - 1)
    step = tp_exchange(0, lambda peer: agx.at[me_t], agx)

    slots = EP * cap
    slot = lax.broadcasted_iota(jnp.int32, (slots, group), 0)
    block = jnp.zeros((slots, group), jnp.int32)
    for j in range(1, EP):
        block = block + jnp.where(slot >= j * cap, 1, 0)
    expert = block * T + me_t
    place = (slot - block * cap).astype(F32)
    hit = jnp.zeros((slots, group), F32)
    weight = jnp.zeros((slots, group), F32)
    for k in range(ids.shape[0]):
        same = ids[k : k + 1, :] == expert
        hit = hit + jnp.where(same, 1.0, 0.0)
        weight = weight + jnp.where(same, wts[k : k + 1, :], 0.0)
    upper = jnp.where(
        lax.broadcasted_iota(jnp.int32, (group, group), 0)
        < lax.broadcasted_iota(jnp.int32, (group, group), 1),
        1.0,
        0.0,
    ).astype(BF16)
    rank = nn(hit.astype(BF16), upper)
    dispatch = jnp.where(rank == place, hit, 0.0)
    weight = weight * dispatch
    weight_hi = weight.astype(BF16)
    weight_lo = (weight - weight_hi.astype(F32)).astype(BF16)
    dispatch = dispatch.astype(BF16)

    for i in range(first_cl):
        loads[i].wait()
    left = jnp.zeros((own, lanes), jnp.int32)
    row = lax.broadcasted_iota(jnp.int32, (own, lanes), 0)
    for b in range(own):
        left = jnp.where(row == b, lengths[b], left)
    length = left
    bits = turns.shape[0] // 2
    cosine = jnp.ones((own, lanes), F32)
    sine = jnp.zeros((own, lanes), F32)
    for i in range(bits - 1, -1, -1):
        has = left >= 2**i
        left = jnp.where(has, left - 2**i, left)
        c, s = turns[i : i + 1, :], turns[bits + i : bits + i + 1, :]
        cosine, sine = (
            jnp.where(has, cosine * c - sine * s, cosine),
            jnp.where(has, cosine * s + sine * c, sine),
        )
    live = lax.broadcasted_iota(jnp.int32, (own, lanes), 1) < rope
    cosine = jnp.where(live, cosine, 0.0)
    sine = jnp.where(live, sine, 0.0)
    big = T * H
    at = lax.broadcasted_iota(jnp.int32, (own * big, own * big), 0)
    to = lax.broadcasted_iota(jnp.int32, (own * big, own * big), 1)

    def from_row(r):
        seq = jnp.zeros_like(r)
        for i in range(1, own):
            seq = seq + jnp.where(r >= i * big, 1, 0)
        return (r - seq * big) * own + seq

    to_seq = jnp.where(to == from_row(at), 1.0, 0.0).astype(BF16)
    to_dev = jnp.where(at == from_row(to), 1.0, 0.0).astype(BF16)
    kr_pad[...] = jnp.zeros_like(kr_pad)
    kr_pad[:, 0:rope] = nt(normed, v_kr[...])
    new_rope = turn(kr_pad[...], cosine, sine, rope // 2).astype(BF16)
    newrope[...] = new_rope[:, 0:rope]

    arrive(step)
    rows = rows_of(agx, T).astype(BF16)
    proj = nt(rows, v_in[...])
    q_lat = [
        nn(lane_block(proj, h * nope, nope)[:, 0:nope].astype(BF16), v_ku[h]) for h in range(H)
    ]
    q_rope = [lane_block(proj, n_q + h * rope, rope) for h in range(H)]
    lat_part = pltpu.roll(lane_block(proj, n_q + n_r, lat_w), lanes - lat_w, 1)
    for u in range(T):
        cut = slice(own * u, own * (u + 1))
        sendq[u, :, 0:latent] = join([q[cut] for q in q_lat]).astype(BF16)
        sendq[u, :, latent : latent + lanes] = join(
            [q[cut] + lat_part[cut] for q in q_rope]
        ).astype(BF16)
    step = tp_exchange(1, lambda peer: sendq.at[peer], recvq)
    recvq[me_t] = sendq[me_t]
    for i in range(first_cl, first_ffn):
        loads[i].wait()
    arrive(step)

    queries = rows_of(recvq, T)
    per = lanes // lat_w
    lane = lax.broadcasted_iota(jnp.int32, (own, lanes), 1)
    blocks = []
    for j in range(T // per):
        total = None
        for i in range(per):
            top = R * (j * per + i)
            piece = jnp.where(lane >= lanes - lat_w, queries[top : top + own, latent:], 0.0)
            if i < per - 1:
                piece = pltpu.roll(piece, (i + 1) * lat_w, 1)
            total = piece if total is None else total + piece
        blocks.append(total)
    raw = blocks[0] if len(blocks) == 1 else jnp.concatenate(blocks, axis=1)
    new_latent = (raw * factor_of(raw) * flat(latent_gain[...])).astype(BF16)
    newlat[...] = new_latent
    new_lat32, new_rope32 = new_latent.astype(F32), new_rope.astype(F32)
    queries = nn(to_seq, queries.astype(BF16))
    q_rot = turn(
        jnp.where(
            lax.broadcasted_iota(jnp.int32, (own * big, lanes), 1) < rope, queries[:, latent:], 0.0
        ),
        spread(cosine, big),
        spread(sine, big),
        rope // 2,
    ).astype(BF16)
    q_lat32 = queries[:, 0:latent]
    outs = []
    for b in range(own):
        cut = slice(big * b, big * (b + 1))
        q_b, r_b = q_lat32[cut], q_rot.astype(F32)[cut]
        lat_b, rope_b = new_lat32[b : b + 1], new_rope32[b : b + 1]
        own_score = (
            jnp.sum(q_b * lat_b, axis=-1, keepdims=True)
            + jnp.sum(r_b * rope_b, axis=-1, keepdims=True)
        ) * scale
        scores = nt(q_b.astype(BF16), v_cl[b]) + nn(r_b[:, 0:rope].astype(BF16), v_cr[b])
        position = lax.broadcasted_iota(jnp.int32, scores.shape, 1)
        scores = jnp.where(position < length[b : b + 1, 0:1], scores * scale, -jnp.inf)
        peak = jnp.maximum(jnp.max(scores, axis=-1, keepdims=True), own_score)
        past = jnp.exp(scores - peak)
        own_exp = jnp.exp(own_score - peak)
        total = jnp.sum(past, axis=-1, keepdims=True) + own_exp
        past = (past / total).astype(BF16)
        own_weight = (own_exp / total).astype(BF16).astype(F32)
        outs.append(nn(past, v_cl[b]) + own_weight * lat_b)
    mixed_lat = nn(to_dev, join(outs).astype(BF16))
    for u in range(T):
        sendo[u] = mixed_lat[R * u : R * (u + 1)].astype(BF16)
    step = tp_exchange(2, lambda peer: sendo.at[peer], recvo)
    recvo[me_t] = sendo[me_t]
    arrive(step)

    back = rows_of(recvo, T).astype(BF16)
    part = None
    for h in range(H):
        values = nt(back, v_vu[h])
        values = join(
            [values[R * u + own * h : R * u + own * (h + 1)] for u in range(T)]
        ).astype(BF16)
        term = nn(values, v_wo[h])
        part = term if part is None else part + term
    for u in range(T):
        senda[u] = part[own * u : own * (u + 1)].astype(BF16)
    step = tp_exchange(3, lambda peer: senda.at[peer], recva)
    recva[me_t] = senda[me_t]
    arrive(step)
    after = tokens[...].astype(F32)
    for u in range(T):
        after = after + recva[u].astype(F32)
    agf[me_t] = (after * factor_of(after) * flat(ffn_gain[...])).astype(BF16)
    step = tp_exchange(4, lambda peer: agf.at[me_t], agf)
    for i in range(first_ffn, len(loads)):
        loads[i].wait()
    arrive(step)

    rows32 = rows_of(agf, T)
    rows = rows32.astype(BF16)
    outgoing = nn(dispatch, rows)
    for j in range(EP):
        sende[j] = outgoing[cap * j : cap * (j + 1)].astype(BF16)
    step = ep_exchange(0, sende, recve)
    recve[me_e] = sende[me_e]

    act = (silu(nt(rows, v_sg[...])) * nt(rows, v_su[...])).astype(BF16)
    ffn = nn(act, v_sd[...])
    gate = jnp.sum(rows32 * flat(branch_gate[...].astype(F32)), axis=-1, keepdims=True)
    gate = 1.0 / (1.0 + jnp.exp(-gate))
    act = (silu(nn(rows, v_dg[...])) * nn(rows, v_du[...])).astype(BF16)
    ffn = ffn + gate * nn(act, v_dd[...])

    arrive(step)
    routed = rows_of(recve, EP).astype(BF16)
    act = (silu(nn(routed, v_eg[...])) * nn(routed, v_eu[...])).astype(BF16)
    result = nn(act, v_ed[...])
    for j in range(EP):
        sendr[j] = result[cap * j : cap * (j + 1)].astype(BF16)
    step = ep_exchange(1, sendr, recvr)
    recvr[me_e] = sendr[me_e]
    arrive(step)
    returned = rows_of(recvr, EP).astype(BF16)
    ffn = ffn + (tn(weight_hi, returned) + tn(weight_lo, returned))
    for u in range(T):
        sendf[u] = ffn[own * u : own * (u + 1)].astype(BF16)
    step = tp_exchange(5, lambda peer: sendf.at[peer], recvf)
    recvf[me_t] = sendf[me_t]
    arrive(step)
    for u in range(T):
        after = after + recvf[u].astype(F32)
    mixed[...] = after.astype(BF16)
    for c in sends:
        c.wait_send()


def hand_over(*refs):
    half = len(refs) // 2
    for source, target in zip(refs[:half], refs[half:]):
        target[...] = source[...]


def local(
    tokens, lengths, cache_latent, cache_rope_key, route_ids, route_weights, attn_gain,
    w_query_nope, w_query_rope, w_latent_down, w_key_rope, latent_gain, w_key_up, w_value_up,
    w_attn_out, ffn_gain, expert_gate, expert_up, expert_down, shared_gate, shared_up,
    shared_down, dense_gate, dense_up, dense_down, branch_gate,
):
    own, width = tokens.shape
    T = lax.axis_size("tp")
    EP = lax.axis_size("ep")
    H, nope = w_query_nope.shape[1:]
    rope = w_query_rope.shape[2]
    latent = cache_latent.shape[2]
    top = route_ids.shape[1]
    assert expert_gate.shape[0] == 1
    cap = max(2, (2 * own * top + EP - 1) // EP)
    R = H * own
    half = rope // 2

    bits = cache_latent.shape[1].bit_length()
    frequencies = (rope_base ** (-np.arange(half) / half)).astype(np.float32).astype(np.float64)
    angles = frequencies[None, :] * 2.0 ** np.arange(bits)[:, None]
    angles = np.pad(np.tile(angles, (1, 2)), ((0, 0), (0, lanes - rope)))
    turns = jnp.asarray(np.concatenate([np.cos(angles), np.sin(angles)]), F32)

    operands = (
        turns,
        tokens,
        route_ids.T,
        route_weights.T,
        attn_gain.reshape(-1, lanes),
        ffn_gain.reshape(-1, lanes),
        latent_gain.reshape(-1, lanes),
        branch_gate.reshape(-1, lanes),
        lengths,
        w_query_nope.transpose(1, 2, 0).reshape(H * nope, width),
        w_query_rope.transpose(1, 2, 0).reshape(H * rope, width),
        w_latent_down.T,
        w_key_rope.T,
        cache_latent,
        cache_rope_key.transpose(0, 2, 1),
        w_key_up.transpose(1, 2, 0),
        w_value_up.transpose(1, 2, 0),
        w_attn_out,
        shared_gate.T,
        shared_up.T,
        dense_gate,
        dense_up,
        shared_down,
        dense_down,
        expert_gate[0],
        expert_up[0],
        expert_down[0],
    )
    big = operands[9:]
    v_in = pltpu.VMEM((sum(o.shape[0] for o in big[:3]), width), BF16)
    weights = [v_in] + [pltpu.VMEM(o.shape, BF16) for o in big[3:]]
    q_width = latent + lanes

    def comm(*shape):
        return pltpu.VMEM(shape, BF16)

    buffers = [
        comm(T, own, width),
        comm(T, R, q_width), comm(T, R, q_width),
        comm(T, R, latent), comm(T, R, latent),
        comm(T, own, width), comm(T, own, width),
        comm(T, own, width),
        comm(EP, cap, width), comm(EP, cap, width),
        comm(EP, cap, width), comm(EP, cap, width),
        comm(T, own, width), comm(T, own, width),
        pltpu.VMEM((own, lanes), F32),
    ]
    n_loads = len(big) + own - 1
    sems = [
        pltpu.SemaphoreType.DMA((n_loads,)),
        pltpu.SemaphoreType.DMA((6, T)),
        pltpu.SemaphoreType.DMA((6, T)),
        pltpu.SemaphoreType.DMA((2, EP)),
        pltpu.SemaphoreType.DMA((2, EP)),
    ]
    sizes = (T, EP, own, H, nope, rope, latent, cap, (nope + rope) ** (-0.5))
    vmem = pl.BlockSpec(memory_space=pltpu.VMEM)
    results = pl.pallas_call(
        functools.partial(layer, sizes),
        out_shape=(
            jax.ShapeDtypeStruct((own, width), BF16),
            jax.ShapeDtypeStruct((own, latent), BF16),
            jax.ShapeDtypeStruct((own, rope), BF16),
        ),
        in_specs=[vmem] * 8
        + [pl.BlockSpec(memory_space=pltpu.SMEM)]
        + [pl.BlockSpec(memory_space=pl.ANY)] * len(big),
        out_specs=(vmem, vmem, vmem),
        scratch_shapes=weights + buffers + sems,
        compiler_params=pltpu.CompilerParams(collective_id=0, has_side_effects=True),
    )(*operands)
    return pl.pallas_call(
        hand_over,
        out_shape=tuple(jax.ShapeDtypeStruct(r.shape, r.dtype) for r in results),
        in_specs=[vmem] * 3,
        out_specs=(vmem, vmem, vmem),
    )(*results)


def solution(mesh):
    both = ("ep", "tp")
    in_specs = (
        P(both, None),
        P(both),
        P(both, None, None),
        P(both, None, None),
        P("ep", None),
        P("ep", None),
        P(),
        P(None, "tp", None),
        P(None, "tp", None),
        P(None, "tp"),
        P(),
        P(),
        P(None, "tp", None),
        P(None, "tp", None),
        P("tp", None, None),
        P(),
        P(both, None, None),
        P(both, None, None),
        P(both, None, None),
        P(None, "tp"),
        P(None, "tp"),
        P("tp", None),
        P(None, "tp"),
        P(None, "tp"),
        P("tp", None),
        P(),
    )
    out_specs = (P(both, None), P(both, None), P(both, None))
    return jax.shard_map(local, mesh=mesh, in_specs=in_specs, out_specs=out_specs, check_vma=False)
```

```python
import functools

import jax
import jax.numpy as jnp
import numpy as np
from jax import lax
from jax.experimental import pallas as pl
from jax.experimental.pallas import tpu as pltpu
from jax.sharding import PartitionSpec as P

epsilon = 1e-06
rope_base = 10000.0
lanes = 128
F32 = jnp.float32
BF16 = jnp.bfloat16
MESH = pl.DeviceIdType.MESH


def nn(a, b):
    return lax.dot_general(a, b, (((1,), (0,)), ((), ())), preferred_element_type=F32)


def nt(a, b):
    return lax.dot_general(a, b, (((1,), (1,)), ((), ())), preferred_element_type=F32)


def tn(a, b):
    return lax.dot_general(a, b, (((0,), (0,)), ((), ())), preferred_element_type=F32)


def join(pieces):
    return pieces[0] if len(pieces) == 1 else jnp.concatenate(pieces, axis=0)


def flipped(index, mask, count):
    out = index
    bit = 1
    while bit < count:
        if mask & bit:
            out = out + bit - 2 * bit * (index // bit % 2)
        bit *= 2
    return out


def flat(ref):
    return jnp.concatenate([ref[i : i + 1, :] for i in range(ref.shape[0])], axis=1)


def spread(values, count):
    rows = values.shape[0]
    return join(
        [jnp.broadcast_to(values[b : b + 1], (count, values.shape[1])) for b in range(rows)]
    )


def rows_of(ref, count):
    return join([ref[i].astype(F32) for i in range(count)])


def factor_of(values):
    return lax.rsqrt(jnp.mean(values * values, axis=-1, keepdims=True) + epsilon)


def silu(v):
    return v / (1.0 + jnp.exp(-v))


def lane_block(values, column, width):
    base, offset = column // lanes * lanes, column % lanes
    block = values[:, base : base + lanes]
    if offset:
        block = pltpu.roll(block, lanes - offset, 1)
    lane = lax.broadcasted_iota(jnp.int32, block.shape, 1)
    return jnp.where(lane < width, block, 0.0)


def turn(values, cosine, sine, half):
    lane = lax.broadcasted_iota(jnp.int32, values.shape, 1)
    swapped = jnp.where(
        lane < half, -pltpu.roll(values, lanes - half, 1), pltpu.roll(values, half, 1)
    )
    return values * cosine + swapped * sine


def layer(
    sizes,
    turns, tokens, ids, wts, attn_gain, ffn_gain, latent_gain, branch_gate, lengths,
    wqn, wqr, wld, wkr, cl, cr, wku, wvu, wo, sg, su, dg, du, sd, dd, eg, eu, ed,
    mixed, newlat, newrope,
    v_in, v_kr, v_cl, v_cr, v_ku, v_vu, v_wo, v_sg, v_su, v_dg, v_du, v_sd, v_dd, v_eg, v_eu, v_ed,
    agx, sendq, recvq, sendo, recvo, senda, recva, agf, sende, recve, sendr, recvr, sendf, recvf,
    half_a, whole_a,
    kr_pad, w_sem, tp_send, tp_recv, ep_send, ep_recv,
):
    T, EP, own, H, nope, rope, latent, cap, scale = sizes
    group = T * own
    R = H * own
    me_t = lax.axis_index("tp")
    me_e = lax.axis_index("ep")
    lat_w = wld.shape[0]

    barrier = pltpu.get_barrier_semaphore()
    for k in range(1, T):
        pl.semaphore_signal(
            barrier, inc=1, device_id=(me_e, flipped(me_t, k, T)), device_id_type=MESH
        )
    for k in range(1, EP):
        pl.semaphore_signal(
            barrier, inc=1, device_id=(flipped(me_e, k, EP), me_t), device_id_type=MESH
        )

    n_q, n_r = H * nope, H * rope
    pairs = [
        (wqn, v_in.at[pl.ds(0, n_q)]),
        (wqr, v_in.at[pl.ds(n_q, n_r)]),
        (wld, v_in.at[pl.ds(n_q + n_r, lat_w)]),
        (wkr, v_kr),
        (wku, v_ku),
    ]
    first_cl = len(pairs)
    pairs += [(cl.at[b], v_cl.at[b]) for b in range(own)]
    first_rest = len(pairs)
    pairs += [(cr, v_cr), (wvu, v_vu), (wo, v_wo)]
    first_ffn = len(pairs)
    pairs += [
        (sg, v_sg), (su, v_su), (dg, v_dg), (du, v_du), (sd, v_sd), (dd, v_dd),
        (eg, v_eg), (eu, v_eu), (ed, v_ed),
    ]
    loads = [
        pltpu.make_async_copy(src, dst, w_sem.at[i]) for i, (src, dst) in enumerate(pairs)
    ]
    for load in loads:
        load.start()

    sends = []

    def tp_exchange(phase, source, target):
        out = []
        for k in range(T - 1, 0, -1):
            peer = flipped(me_t, k, T)
            out.append(
                pltpu.make_async_remote_copy(
                    src_ref=source(peer),
                    dst_ref=target.at[me_t],
                    send_sem=tp_send.at[phase, k],
                    recv_sem=tp_recv.at[phase, k],
                    device_id=(me_e, peer),
                    device_id_type=MESH,
                )
            )
        for c in out:
            c.start()
        sends.extend(out)
        return out

    def tp_copy(phase, k, source, target, peer):
        c = pltpu.make_async_remote_copy(
            src_ref=source,
            dst_ref=target,
            send_sem=tp_send.at[phase, k],
            recv_sem=tp_recv.at[phase, k],
            device_id=(me_e, peer),
            device_id_type=MESH,
        )
        c.start()
        sends.append(c)
        return c

    partner = flipped(me_t, 1, T)
    across = list(range(T - 2, 0, -2))

    def tp_gather(phase, target):
        mine = target.at[me_t]
        direct = [(m, tp_copy(phase, m, mine, mine, flipped(me_t, m, T))) for m in across]
        out = [tp_copy(phase, 1, mine, mine, partner)]

        def finish():
            for m, c in reversed(direct):
                c.wait_recv()
                block = target.at[flipped(me_t, m, T)]
                out.append(tp_copy(phase, m + 1, block, block, partner))
            for c in out:
                c.wait_recv()

        return finish

    def tp_scatter(phase, source, half, whole, target):
        first = []
        for m in across + [0]:
            to = flipped(partner, m, T)
            first.append((m, tp_copy(phase, m + 1, source.at[to], half.at[to], partner)))
        out = []
        for m, c in first:
            c.wait_recv()
            to = flipped(me_t, m, T)
            both = (source[to].astype(F32) + half[to].astype(F32)).astype(BF16)
            if m == 0:
                target[me_t] = both
            else:
                whole[to] = both
                out.append(tp_copy(phase, m, whole.at[to], target.at[me_t], to))
        for c in out:
            c.wait_recv()
        total = target[me_t].astype(F32)
        for m in across:
            total = total + target[flipped(me_t, m, T)].astype(F32)
        return total

    def ep_exchange(phase, source, target):
        out = []
        for k in range(EP - 1, 0, -1):
            peer = flipped(me_e, k, EP)
            out.append(
                pltpu.make_async_remote_copy(
                    src_ref=source.at[peer],
                    dst_ref=target.at[me_e],
                    send_sem=ep_send.at[phase, k],
                    recv_sem=ep_recv.at[phase, k],
                    device_id=(peer, me_t),
                    device_id_type=MESH,
                )
            )
        for c in out:
            c.start()
        sends.extend(out)
        return out

    def arrive(copies):
        for c in copies:
            c.wait_recv()

    x = tokens[...].astype(F32)
    normed = (x * factor_of(x) * flat(attn_gain[...])).astype(BF16)
    agx[me_t] = normed
    pl.semaphore_wait(barrier, T - 1 + EP - 1)
    finish = tp_gather(0, agx)

    slots = EP * cap
    slot = lax.broadcasted_iota(jnp.int32, (slots, group), 0)
    block = jnp.zeros((slots, group), jnp.int32)
    for j in range(1, EP):
        block = block + jnp.where(slot >= j * cap, 1, 0)
    expert = block * T + me_t
    place = (slot - block * cap).astype(F32)
    hit = jnp.zeros((slots, group), F32)
    weight = jnp.zeros((slots, group), F32)
    for k in range(ids.shape[0]):
        same = ids[k : k + 1, :] == expert
        hit = hit + jnp.where(same, 1.0, 0.0)
        weight = weight + jnp.where(same, wts[k : k + 1, :], 0.0)
    upper = jnp.where(
        lax.broadcasted_iota(jnp.int32, (group, group), 0)
        < lax.broadcasted_iota(jnp.int32, (group, group), 1),
        1.0,
        0.0,
    ).astype(BF16)
    rank = nn(hit.astype(BF16), upper)
    dispatch = jnp.where(rank == place, hit, 0.0)
    weight = weight * dispatch
    weight_hi = weight.astype(BF16)
    weight_lo = (weight - weight_hi.astype(F32)).astype(BF16)
    dispatch = dispatch.astype(BF16)

    for i in range(first_cl):
        loads[i].wait()
    left = jnp.zeros((own, lanes), jnp.int32)
    row = lax.broadcasted_iota(jnp.int32, (own, lanes), 0)
    for b in range(own):
        left = jnp.where(row == b, lengths[b], left)
    length = left
    bits = turns.shape[0] // 2
    cosine = jnp.ones((own, lanes), F32)
    sine = jnp.zeros((own, lanes), F32)
    for i in range(bits - 1, -1, -1):
        has = left >= 2**i
        left = jnp.where(has, left - 2**i, left)
        c, s = turns[i : i + 1, :], turns[bits + i : bits + i + 1, :]
        cosine, sine = (
            jnp.where(has, cosine * c - sine * s, cosine),
            jnp.where(has, cosine * s + sine * c, sine),
        )
    live = lax.broadcasted_iota(jnp.int32, (own, lanes), 1) < rope
    cosine = jnp.where(live, cosine, 0.0)
    sine = jnp.where(live, sine, 0.0)
    big = T * H
    at = lax.broadcasted_iota(jnp.int32, (own * big, own * big), 0)
    to = lax.broadcasted_iota(jnp.int32, (own * big, own * big), 1)

    def from_row(r):
        seq = jnp.zeros_like(r)
        for i in range(1, own):
            seq = seq + jnp.where(r >= i * big, 1, 0)
        return (r - seq * big) * own + seq

    to_seq = jnp.where(to == from_row(at), 1.0, 0.0).astype(BF16)
    to_dev = jnp.where(at == from_row(to), 1.0, 0.0).astype(BF16)
    kr_pad[...] = jnp.zeros_like(kr_pad)
    kr_pad[:, 0:rope] = nt(normed, v_kr[...])
    new_rope = turn(kr_pad[...], cosine, sine, rope // 2).astype(BF16)
    newrope[...] = new_rope[:, 0:rope]

    finish()
    rows = rows_of(agx, T).astype(BF16)
    proj = nt(rows, v_in[...])
    q_lat = [
        nn(lane_block(proj, h * nope, nope)[:, 0:nope].astype(BF16), v_ku[h]) for h in range(H)
    ]
    q_rope = [lane_block(proj, n_q + h * rope, rope) for h in range(H)]
    lat_part = pltpu.roll(lane_block(proj, n_q + n_r, lat_w), lanes - lat_w, 1)
    for u in range(T):
        cut = slice(own * u, own * (u + 1))
        sendq[u, :, 0:latent] = join([q[cut] for q in q_lat]).astype(BF16)
        sendq[u, :, latent : latent + lanes] = join(
            [q[cut] + lat_part[cut] for q in q_rope]
        ).astype(BF16)
    step = tp_exchange(1, lambda peer: sendq.at[peer], recvq)
    recvq[me_t] = sendq[me_t]
    for i in range(first_cl, first_ffn):
        loads[i].wait()
    arrive(step)

    queries = rows_of(recvq, T)
    per = lanes // lat_w
    lane = lax.broadcasted_iota(jnp.int32, (own, lanes), 1)
    blocks = []
    for j in range(T // per):
        total = None
        for i in range(per):
            top = R * (j * per + i)
            piece = jnp.where(lane >= lanes - lat_w, queries[top : top + own, latent:], 0.0)
            if i < per - 1:
                piece = pltpu.roll(piece, (i + 1) * lat_w, 1)
            total = piece if total is None else total + piece
        blocks.append(total)
    raw = blocks[0] if len(blocks) == 1 else jnp.concatenate(blocks, axis=1)
    new_latent = (raw * factor_of(raw) * flat(latent_gain[...])).astype(BF16)
    newlat[...] = new_latent
    new_lat32, new_rope32 = new_latent.astype(F32), new_rope.astype(F32)
    queries = nn(to_seq, queries.astype(BF16))
    q_rot = turn(
        jnp.where(
            lax.broadcasted_iota(jnp.int32, (own * big, lanes), 1) < rope, queries[:, latent:], 0.0
        ),
        spread(cosine, big),
        spread(sine, big),
        rope // 2,
    ).astype(BF16)
    q_lat32 = queries[:, 0:latent]
    outs = []
    for b in range(own):
        cut = slice(big * b, big * (b + 1))
        q_b, r_b = q_lat32[cut], q_rot.astype(F32)[cut]
        lat_b, rope_b = new_lat32[b : b + 1], new_rope32[b : b + 1]
        own_score = (
            jnp.sum(q_b * lat_b, axis=-1, keepdims=True)
            + jnp.sum(r_b * rope_b, axis=-1, keepdims=True)
        ) * scale
        scores = nt(q_b.astype(BF16), v_cl[b]) + nn(r_b[:, 0:rope].astype(BF16), v_cr[b])
        position = lax.broadcasted_iota(jnp.int32, scores.shape, 1)
        scores = jnp.where(position < length[b : b + 1, 0:1], scores * scale, -jnp.inf)
        peak = jnp.maximum(jnp.max(scores, axis=-1, keepdims=True), own_score)
        past = jnp.exp(scores - peak)
        own_exp = jnp.exp(own_score - peak)
        total = jnp.sum(past, axis=-1, keepdims=True) + own_exp
        past = (past / total).astype(BF16)
        own_weight = (own_exp / total).astype(BF16).astype(F32)
        outs.append(nn(past, v_cl[b]) + own_weight * lat_b)
    mixed_lat = nn(to_dev, join(outs).astype(BF16))
    for u in range(T):
        sendo[u] = mixed_lat[R * u : R * (u + 1)].astype(BF16)
    step = tp_exchange(2, lambda peer: sendo.at[peer], recvo)
    recvo[me_t] = sendo[me_t]
    arrive(step)

    back = rows_of(recvo, T).astype(BF16)
    part = None
    for h in range(H):
        values = nt(back, v_vu[h])
        values = join(
            [values[R * u + own * h : R * u + own * (h + 1)] for u in range(T)]
        ).astype(BF16)
        term = nn(values, v_wo[h])
        part = term if part is None else part + term
    for u in range(T):
        senda[u] = part[own * u : own * (u + 1)].astype(BF16)
    after = tokens[...].astype(F32) + tp_scatter(3, senda, half_a, whole_a, recva)
    agf[me_t] = (after * factor_of(after) * flat(ffn_gain[...])).astype(BF16)
    finish = tp_gather(4, agf)
    for i in range(first_ffn, len(loads)):
        loads[i].wait()
    finish()

    rows32 = rows_of(agf, T)
    rows = rows32.astype(BF16)
    outgoing = nn(dispatch, rows)
    for j in range(EP):
        sende[j] = outgoing[cap * j : cap * (j + 1)].astype(BF16)
    step = ep_exchange(0, sende, recve)
    recve[me_e] = sende[me_e]

    act = (silu(nt(rows, v_sg[...])) * nt(rows, v_su[...])).astype(BF16)
    ffn = nn(act, v_sd[...])
    gate = jnp.sum(rows32 * flat(branch_gate[...].astype(F32)), axis=-1, keepdims=True)
    gate = 1.0 / (1.0 + jnp.exp(-gate))
    act = (silu(nn(rows, v_dg[...])) * nn(rows, v_du[...])).astype(BF16)
    ffn = ffn + gate * nn(act, v_dd[...])

    arrive(step)
    routed = rows_of(recve, EP).astype(BF16)
    act = (silu(nn(routed, v_eg[...])) * nn(routed, v_eu[...])).astype(BF16)
    wide = v_ed.shape[1] // 2
    cuts = [slice(0, wide), slice(wide, 2 * wide)]
    steps = []
    for n, cut in enumerate(cuts):
        result = nn(act, v_ed[:, cut])
        for j in range(EP):
            sendr[n, j] = result[cap * j : cap * (j + 1)].astype(BF16)
        steps.append(ep_exchange(1 + n, sendr.at[n], recvr.at[n]))
        recvr[n, me_e] = sendr[n, me_e]
    last = []
    for n, cut in enumerate(cuts):
        arrive(steps[n])
        returned = rows_of(recvr.at[n], EP).astype(BF16)
        part = ffn[:, cut] + (tn(weight_hi, returned) + tn(weight_lo, returned))
        for u in range(T):
            sendf[n, u] = part[own * u : own * (u + 1)].astype(BF16)
        last.append(tp_exchange(5 + n, lambda peer: sendf.at[n, peer], recvf.at[n]))
        recvf[n, me_t] = sendf[n, me_t]
    for n, cut in enumerate(cuts):
        arrive(last[n])
        part = after[:, cut]
        for u in range(T):
            part = part + recvf[n, u].astype(F32)
        mixed[:, cut] = part.astype(BF16)
    for c in sends:
        c.wait_send()


def hand_over(*refs):
    half = len(refs) // 2
    for source, target in zip(refs[:half], refs[half:]):
        target[...] = source[...]


def local(
    tokens, lengths, cache_latent, cache_rope_key, route_ids, route_weights, attn_gain,
    w_query_nope, w_query_rope, w_latent_down, w_key_rope, latent_gain, w_key_up, w_value_up,
    w_attn_out, ffn_gain, expert_gate, expert_up, expert_down, shared_gate, shared_up,
    shared_down, dense_gate, dense_up, dense_down, branch_gate,
):
    own, width = tokens.shape
    T = lax.axis_size("tp")
    EP = lax.axis_size("ep")
    H, nope = w_query_nope.shape[1:]
    rope = w_query_rope.shape[2]
    latent = cache_latent.shape[2]
    top = route_ids.shape[1]
    assert expert_gate.shape[0] == 1
    cap = max(2, (2 * own * top + EP - 1) // EP)
    R = H * own
    half = rope // 2

    bits = cache_latent.shape[1].bit_length()
    frequencies = (rope_base ** (-np.arange(half) / half)).astype(np.float32).astype(np.float64)
    angles = frequencies[None, :] * 2.0 ** np.arange(bits)[:, None]
    angles = np.pad(np.tile(angles, (1, 2)), ((0, 0), (0, lanes - rope)))
    turns = jnp.asarray(np.concatenate([np.cos(angles), np.sin(angles)]), F32)

    operands = (
        turns,
        tokens,
        route_ids.T,
        route_weights.T,
        attn_gain.reshape(-1, lanes),
        ffn_gain.reshape(-1, lanes),
        latent_gain.reshape(-1, lanes),
        branch_gate.reshape(-1, lanes),
        lengths,
        w_query_nope.transpose(1, 2, 0).reshape(H * nope, width),
        w_query_rope.transpose(1, 2, 0).reshape(H * rope, width),
        w_latent_down.T,
        w_key_rope.T,
        cache_latent,
        cache_rope_key.transpose(0, 2, 1),
        w_key_up.transpose(1, 2, 0),
        w_value_up.transpose(1, 2, 0),
        w_attn_out,
        shared_gate.T,
        shared_up.T,
        dense_gate,
        dense_up,
        shared_down,
        dense_down,
        expert_gate[0],
        expert_up[0],
        expert_down[0],
    )
    big = operands[9:]
    v_in = pltpu.VMEM((sum(o.shape[0] for o in big[:3]), width), BF16)
    weights = [v_in] + [pltpu.VMEM(o.shape, BF16) for o in big[3:]]
    q_width = latent + lanes

    def comm(*shape):
        return pltpu.VMEM(shape, BF16)

    buffers = [
        comm(T, own, width),
        comm(T, R, q_width), comm(T, R, q_width),
        comm(T, R, latent), comm(T, R, latent),
        comm(T, own, width), comm(T, own, width),
        comm(T, own, width),
        comm(EP, cap, width), comm(EP, cap, width),
        comm(2, EP, cap, width // 2), comm(2, EP, cap, width // 2),
        comm(2, T, own, width // 2), comm(2, T, own, width // 2),
        comm(T, own, width), comm(T, own, width),
        pltpu.VMEM((own, lanes), F32),
    ]
    n_loads = len(big) + own - 1
    sems = [
        pltpu.SemaphoreType.DMA((n_loads,)),
        pltpu.SemaphoreType.DMA((7, T)),
        pltpu.SemaphoreType.DMA((7, T)),
        pltpu.SemaphoreType.DMA((3, EP)),
        pltpu.SemaphoreType.DMA((3, EP)),
    ]
    sizes = (T, EP, own, H, nope, rope, latent, cap, (nope + rope) ** (-0.5))
    vmem = pl.BlockSpec(memory_space=pltpu.VMEM)
    results = pl.pallas_call(
        functools.partial(layer, sizes),
        out_shape=(
            jax.ShapeDtypeStruct((own, width), BF16),
            jax.ShapeDtypeStruct((own, latent), BF16),
            jax.ShapeDtypeStruct((own, rope), BF16),
        ),
        in_specs=[vmem] * 8
        + [pl.BlockSpec(memory_space=pltpu.SMEM)]
        + [pl.BlockSpec(memory_space=pl.ANY)] * len(big),
        out_specs=(vmem, vmem, vmem),
        scratch_shapes=weights + buffers + sems,
        compiler_params=pltpu.CompilerParams(collective_id=0, has_side_effects=True),
    )(*operands)
    return pl.pallas_call(
        hand_over,
        out_shape=tuple(jax.ShapeDtypeStruct(r.shape, r.dtype) for r in results),
        in_specs=[vmem] * 3,
        out_specs=(vmem, vmem, vmem),
    )(*results)


def solution(mesh):
    both = ("ep", "tp")
    in_specs = (
        P(both, None),
        P(both),
        P(both, None, None),
        P(both, None, None),
        P("ep", None),
        P("ep", None),
        P(),
        P(None, "tp", None),
        P(None, "tp", None),
        P(None, "tp"),
        P(),
        P(),
        P(None, "tp", None),
        P(None, "tp", None),
        P("tp", None, None),
        P(),
        P(both, None, None),
        P(both, None, None),
        P(both, None, None),
        P(None, "tp"),
        P(None, "tp"),
        P("tp", None),
        P(None, "tp"),
        P(None, "tp"),
        P("tp", None),
        P(),
    )
    out_specs = (P(both, None), P(both, None), P(both, None))
    return jax.shard_map(local, mesh=mesh, in_specs=in_specs, out_specs=out_specs, check_vma=False)
```
